32 devices in a mesh: ep: 32 (over z, y, x, core).
Axes of the slice: x: 2, y: 2, z: 4, core: 2. Of those that a mesh axis runs over, the one named last changes fastest.
Arguments:
- tokens: bfloat16 [576, 2048], P('ep'), may hold values from -6 to 6
- attn_norm_gain: float32 [2048], replicated, may hold values from 0.1 to 1.9
- w_query: bfloat16 [2048, 512], replicated, may hold values from -0.125 to 0.125
- w_key: bfloat16 [2048, 128], replicated, may hold values from -0.125 to 0.125
- w_value: bfloat16 [2048, 128], replicated, may hold values from -0.125 to 0.125
- w_forget: bfloat16 [2048, 8], replicated, may hold values from -0.125 to 0.125
- forget_bias: float32 [8], replicated, may hold values from 0.5 to 4
- w_attn_out: bfloat16 [512, 2048], replicated, may hold values from -0.25 to 0.25
- cache_keys: bfloat16 [576, 1024, 128], P('ep'), may hold values from -72 to 72
- cache_values: bfloat16 [576, 1024, 128], P('ep'), may hold values from -6 to 6
- cache_logcum: float32 [576, 8, 1024], P('ep'), as said below
- cache_lengths: int32 [576], P('ep'), may hold values from 128 to 1024
- expert_norm_gain: float32 [2048], replicated, may hold values from 0.4 to 40
- expert_ids: int32 [576, 6], P('ep'), may hold values from 0 to 31, all different within a row; in each aligned block of 18 rows (0 to 17, 18 to 35, ...) at most 6 rows name the same one
- expert_weights: float32 [576, 6], P('ep'), may hold values from 0.1 to 1
- w_expert_gate: bfloat16 [32, 2048, 512], P('ep'), may hold values from -0.125 to 0.125
- w_expert_up: bfloat16 [32, 2048, 512], P('ep'), may hold values from -0.125 to 0.125
- w_expert_down: bfloat16 [32, 512, 2048], P('ep'), may hold values from -0.25 to 0.25
- w_dense_gate: bfloat16 [2048, 4096], P(None, 'ep'), may hold values from -0.125 to 0.125
- w_dense_up: bfloat16 [2048, 4096], P(None, 'ep'), may hold values from -2 to 2
- w_dense_down: bfloat16 [4096, 2048], P('ep'), may hold values from -0.09375 to 0.09375
- dense_norm_gain: float32 [4096], replicated, may hold values from 0.1 to 1.9
- branch_gate: float32 [2048], replicated, may hold values from -0.125 to 0.125
Outputs:
- result: bfloat16 [576, 2048], P('ep')
The draws below stay inside these ranges and needn't reach their ends.
Inputs may be any that keep to these rules, and one draw needn't show every extreme that they name: `cache_logcum`: along the positions of each sequence and head the values never rise. `expert_ids`: each row names 6 different experts; among the rows of one device no expert is named by more than 6 rows, and in every draw some device names some expert exactly 6 times.
All inputs are finite; a program needn't handle non-finite values.
Results may differ from the reference program's by a relative error of at most 0.012.
The reference program's roundings to bfloat16 on the way count: a program that leaves them out, or rounds other values in their place, can miss the bound.
Values may be sent and summed in bfloat16 or wider, within the bound.
A program may use at most 128 MiB of HBM per device.

```python
import math
import jax
import jax.numpy as jnp
import numpy as np
from jax import lax

D = 2048
HEADS = 8
KV_HEADS = 2
HEAD_DIM = 64
EXPERT_FF = 512
DENSE_FF = 4096
TOPK = 6
SEQ_DEV = 18
CACHE_POSITIONS = 1024
SEQS = 576
EXPERTS = 32
CAP = 6
N_EP = 32


def draw_cache_keys(key, part):
    tensor_extent = (SEQS, CACHE_POSITIONS, KV_HEADS * HEAD_DIM)
    base = jnp.clip(jax.random.normal(jax.random.fold_in(key, 11), tensor_extent, jnp.float32), -6.0, 6.0)
    values = base
    return jnp.clip(values, -72.0, 72.0).astype(jnp.bfloat16)


def draw_cache_logcum(key, part):
    tensor_extent = (SEQS, HEADS, CACHE_POSITIONS)
    order = jax.random.permutation(jax.random.fold_in(key, 21), HEADS)
    gradual_decay = (order < HEADS // 2)[None, :, None]
    chain_total = jax.random.uniform(jax.random.fold_in(key, 22), (SEQS, HEADS, 1), jnp.float32, 0.3, 1.5)
    fast_span = jax.random.uniform(jax.random.fold_in(key, 23), (SEQS, HEADS, 1), jnp.float32, 30.0, 100.0)
    decay_speed = jnp.where(gradual_decay, chain_total / CACHE_POSITIONS, 1.0 / fast_span)
    sequence_multiplier = jnp.exp(jax.random.uniform(jax.random.fold_in(key, 24), (SEQS, 1, 1), jnp.float32, -0.7, 0.7))
    coarse_estimate = jnp.exp(jax.random.uniform(jax.random.fold_in(key, 25), tensor_extent, jnp.float32, -0.7, 0.7))
    spike_position = jax.random.uniform(jax.random.fold_in(key, 26), tensor_extent, jnp.float32) < 3.0 / CACHE_POSITIONS
    spike_amount = -jnp.log(jax.random.uniform(jax.random.fold_in(key, 27), tensor_extent, jnp.float32, 0.5, 0.8))
    step_numbers = decay_speed * sequence_multiplier * coarse_estimate + jnp.where(spike_position & gradual_decay, spike_amount, 0.0)
    return -jnp.cumsum(step_numbers, axis=2)


def draw_expert_norm_gain(key, part):
    base = 1.0 + 0.18 * jnp.clip(jax.random.normal(jax.random.fold_in(key, 31), (D,), jnp.float32), -3.0, 3.0)
    return base


def draw_w_dense_up(key, part):
    normal_part = jnp.clip(jax.random.normal(jax.random.fold_in(key, 41), (D, DENSE_FF), jnp.float32), -6.0, 6.0)
    column = jnp.arange(DENSE_FF, dtype=jnp.float32)[None, :] / DENSE_FF
    scale = 3.0 ** column * jnp.exp(jax.random.uniform(jax.random.fold_in(key, 43), (1, DENSE_FF), jnp.float32, -0.3, 0.3))
    return jnp.clip(normal_part * D ** (-0.5) * scale, -2.0, 2.0).astype(jnp.bfloat16)


def with_ends(drawn, key, smallest, largest):
    shape = drawn.shape
    spot = [jax.random.randint(jax.random.fold_in(key, axis), (), 0, shape[axis]) for axis in range(len(shape))]
    drawn = drawn.at[tuple(spot)].set(smallest)
    longest = shape.index(max(shape))
    spot[longest] = (spot[longest] + 1) % shape[longest]
    return drawn.at[tuple(spot)].set(largest)


def steps_of(key, extent, cuts, least, top_value):
    factor_of = 1.0
    for axis_at, parts in cuts:
        steps = jax.random.uniform(jax.random.fold_in(jax.random.fold_in(key, 6), axis_at), (parts,), jnp.float32, least / len(cuts), top_value / len(cuts))
        factor_of = factor_of * jnp.repeat(jnp.exp(steps), extent[axis_at] // parts).reshape((-1,) + (1,) * (len(extent) - 1 - axis_at))
    return factor_of


def deal_out(rng, own, number, rows, number_of, top, most, lean):
    sequence = jax.random.permutation(rng, number_of)
    crowded, usual = shares(number_of, rows * top, most, lean, True), shares(number_of, rows * top, most, lean, False)
    places = jnp.arange(number_of)

    def named(tallies, rotation):
        used = int((tallies > 0).sum())
        fixed = max(1, used // 4)
        shifted = fixed + (places - fixed + rotation * (used - fixed)) % max(1, number_of - fixed)
        return jnp.zeros((number_of,), jnp.int32).at[sequence[jnp.where(places < fixed, places, shifted)]].set(jnp.asarray(tallies, jnp.int32))

    tallies = jnp.where(number % 4 == 0, named(crowded, number // 4), named(usual, number - number // 4 - 1))
    mixed = jax.random.permutation(jax.random.fold_in(own, 3), number_of)
    giver, receiver = mixed[0:number_of // 2 * 2:2], mixed[1:number_of // 2 * 2:2]
    margin = jnp.minimum(tallies[giver] - 1, most - tallies[receiver]) // 2
    margin = jnp.where((giver == sequence[0]) | (receiver == sequence[0]) | (tallies[receiver] == 0), 0, jnp.maximum(margin, 0))
    shifted = jax.random.randint(jax.random.fold_in(own, 4), (number_of // 2,), 0, 1 << 20) % (margin + 1)
    tallies = tallies.at[giver].add(-shifted).at[receiver].add(shifted)
    labels = jnp.searchsorted(jnp.cumsum(tallies), jnp.arange(rows * top), side="right").astype(jnp.int32)
    listing = labels.reshape(top, rows).T
    listing = listing[jax.random.permutation(jax.random.fold_in(own, 1), rows)]
    rotation = jax.random.randint(jax.random.fold_in(own, 2), (rows, 1), 0, top)
    return jnp.take_along_axis(listing, (jnp.arange(top)[None, :] + rotation) % top, axis=1)


def shares(number_of, total, limit, skew, full):
    loads = [(1 << 20) // math.isqrt(standing ** skew) + 1 for standing in range(1, number_of + 1)]
    largest = limit if full else min(limit, max(-(-total // number_of), total * loads[0] // sum(loads)))
    least = 1 if total - largest >= number_of - 1 else 0
    given, spare = [largest] + [least] * (number_of - 1), total - largest - least * (number_of - 1)
    while spare > 0:
        candidates = [i for i in range(1, number_of) if given[i] < largest] or [i for i in range(1, number_of) if given[i] < limit]
        whole, budget = sum([loads[i] for i in candidates]), spare
        for i in candidates:
            extra = min(limit - given[i], max(1, budget * loads[i] // whole), spare)
            given[i] = given[i] + extra
            spare = spare - extra
    return np.array(given)


def centred(rng, extent, deviation, bound, shards=(), held_as=jnp.bfloat16):
    values = deviation * jax.random.normal(rng, extent, jnp.float32)
    if shards:
        values = values * steps_of(rng, extent, shards, -0.22, 0.18)
    return jnp.clip(values, -bound, bound).astype(held_as)


def setup_inputs(seed: int = 0) -> dict:
    splits = jax.random.split(jax.random.key(seed), 24)
    tokens = centred(splits[0], (SEQS, D), 1.0, 6.0, ((0, 32),))
    attn_norm_gain = jnp.clip(1.0 + 0.18 * jax.random.normal(splits[1], (D,), jnp.float32), 0.1, 1.9)
    w_query = centred(splits[2], (D, HEADS * HEAD_DIM), D ** -0.5, 0.125)
    w_key = centred(splits[3], (D, KV_HEADS * HEAD_DIM), D ** -0.5, 0.125)
    w_value = centred(splits[4], (D, KV_HEADS * HEAD_DIM), D ** -0.5, 0.125)
    w_forget = centred(splits[5], (D, HEADS), D ** -0.5, 0.125)
    forget_bias = jnp.clip(jax.random.uniform(splits[6], (HEADS,), jnp.float32, 0.5, 4.0), 0.5, 4.0)
    w_attn_out = centred(splits[7], (HEADS * HEAD_DIM, D), (HEADS * HEAD_DIM) ** -0.5, 0.25)
    cache_keys = draw_cache_keys(jax.random.fold_in(splits[23], 71), 0)
    cache_values = centred(splits[9], (SEQS, CACHE_POSITIONS, KV_HEADS * HEAD_DIM), 1.0, 6.0, ((0, 32),))
    cache_logcum = draw_cache_logcum(jax.random.fold_in(splits[23], 71), 0)
    cache_lengths = with_ends(jax.random.randint(splits[11], (SEQS,), CACHE_POSITIONS // 8, CACHE_POSITIONS + 1), jax.random.fold_in(splits[11], 1), CACHE_POSITIONS // 8, CACHE_POSITIONS).astype(jnp.int32)
    expert_norm_gain = draw_expert_norm_gain(jax.random.fold_in(splits[23], 71), 0)
    expert_ids_keys = jax.random.split(jax.random.fold_in(splits[13], 1), SEQS // SEQ_DEV)
    expert_ids_turns = jax.random.permutation(jax.random.fold_in(splits[13], 3), SEQS // SEQ_DEV)
    expert_ids = jax.vmap(lambda own, number: deal_out(jax.random.fold_in(splits[13], 2), own, number, SEQ_DEV, EXPERTS, TOPK, CAP, 2))(expert_ids_keys, expert_ids_turns).reshape((SEQS, TOPK))
    expert_weights = jnp.clip(jnp.exp(math.log(1.0) - 2.3025851 * jax.random.uniform(splits[14], (SEQS, TOPK), jnp.float32) ** steps_of(splits[14], (SEQS, TOPK), ((0, 32),), -0.2, 0.2)), 0.1, 1.0)
    w_expert_gate = centred(splits[15], (EXPERTS, D, EXPERT_FF), D ** -0.5, 0.125, ((0, 32),))
    w_expert_up = centred(splits[16], (EXPERTS, D, EXPERT_FF), D ** -0.5, 0.125, ((0, 32),))
    w_expert_down = centred(splits[17], (EXPERTS, EXPERT_FF, D), EXPERT_FF ** -0.5, 0.25, ((0, 32),))
    w_dense_gate = centred(splits[18], (D, DENSE_FF), D ** -0.5, 0.125, ((1, 32),))
    w_dense_up = draw_w_dense_up(jax.random.fold_in(splits[23], 71), 0)
    w_dense_down = centred(splits[20], (DENSE_FF, D), DENSE_FF ** -0.5, 0.09375, ((0, 32),))
    dense_norm_gain = jnp.clip(1.0 + 0.18 * jax.random.normal(splits[21], (DENSE_FF,), jnp.float32), 0.1, 1.9)
    branch_gate = centred(splits[22], (D,), D ** -0.5, 0.125, (), jnp.float32)
    return dict(tokens=tokens, attn_norm_gain=attn_norm_gain, w_query=w_query, w_key=w_key, w_value=w_value, w_forget=w_forget, forget_bias=forget_bias, w_attn_out=w_attn_out, cache_keys=cache_keys, cache_values=cache_values, cache_logcum=cache_logcum, cache_lengths=cache_lengths, expert_norm_gain=expert_norm_gain, expert_ids=expert_ids, expert_weights=expert_weights, w_expert_gate=w_expert_gate, w_expert_up=w_expert_up, w_expert_down=w_expert_down, w_dense_gate=w_dense_gate, w_dense_up=w_dense_up, w_dense_down=w_dense_down, dense_norm_gain=dense_norm_gain, branch_gate=branch_gate)


EPS = 1e-06
LIMIT = 7.0
ALPHA = 1.702

def normalize(values, gain):
    return values * lax.rsqrt(lax.optimization_barrier(jnp.mean(values * values, axis=-1, keepdims=True)) + EPS) * gain

def stored(values):
    return lax.optimization_barrier(values.astype(jnp.bfloat16))

def attend(query, key_new, value_new, log_forget, cache_keys, cache_values, cache_logcum, cache_lengths):
    seqs, length = (cache_keys.shape[0], cache_keys.shape[1])
    group = HEADS // KV_HEADS
    scale = HEAD_DIM ** (-0.5)
    heads_q = query.astype(jnp.float32).reshape(seqs, KV_HEADS, group, HEAD_DIM)
    keys = cache_keys.astype(jnp.float32).reshape(seqs, length, KV_HEADS, HEAD_DIM)
    values = cache_values.astype(jnp.float32).reshape(seqs, length, KV_HEADS, HEAD_DIM)
    own_key = key_new.astype(jnp.float32).reshape(seqs, KV_HEADS, HEAD_DIM)
    own_value = value_new.astype(jnp.float32).reshape(seqs, KV_HEADS, 1, HEAD_DIM)
    last_index = jnp.broadcast_to((cache_lengths - 1)[:, None, None], (seqs, HEADS, 1)).astype(jnp.int32)
    carried = jnp.take_along_axis(cache_logcum, last_index, axis=2)[:, :, 0] + log_forget
    offset = (carried[:, :, None] - cache_logcum).reshape(seqs, KV_HEADS, group, length)
    scores = jnp.einsum('skgd,slkd->skgl', heads_q, keys) * scale + offset
    live = jnp.arange(length, dtype=jnp.int32)[None, :] < cache_lengths[:, None]
    scores = jnp.where(live[:, None, None, :], scores, -jnp.inf)
    own = jnp.einsum('skgd,skd->skg', heads_q, own_key) * scale
    top = jnp.maximum(lax.optimization_barrier(jnp.max(scores, axis=-1)), own)
    expo = jnp.exp(scores - top[..., None])
    own_expo = jnp.exp(own - top)
    total = lax.optimization_barrier(jnp.sum(expo, axis=-1)) + own_expo
    weights = stored(expo / total[..., None]).astype(jnp.float32)
    own_weight = stored(own_expo / total).astype(jnp.float32)
    out = jnp.einsum('skgl,slkd->skgd', weights, values) + own_weight[..., None] * own_value
    return out.reshape(seqs, HEADS * HEAD_DIM).astype(jnp.bfloat16)

def expert_unit(rows, gate_w, up_w, down_w):
    gate = jnp.minimum(jnp.dot(rows, gate_w, preferred_element_type=jnp.float32), LIMIT)
    up = jnp.clip(jnp.dot(rows, up_w, preferred_element_type=jnp.float32), -LIMIT, LIMIT)
    act = ((up + 1.0) * gate * jax.nn.sigmoid(gate * ALPHA)).astype(jnp.bfloat16)
    return jnp.dot(act, down_w, preferred_element_type=jnp.float32).astype(jnp.bfloat16)

def reference(tokens, attn_norm_gain, w_query, w_key, w_value, w_forget, forget_bias, w_attn_out, cache_keys, cache_values, cache_logcum, cache_lengths, expert_norm_gain, expert_ids, expert_weights, w_expert_gate, w_expert_up, w_expert_down, w_dense_gate, w_dense_up, w_dense_down, dense_norm_gain, branch_gate):
    seqs = tokens.shape[0]
    normed = normalize(tokens.astype(jnp.float32), attn_norm_gain).astype(jnp.bfloat16)
    query = jnp.dot(normed, w_query, preferred_element_type=jnp.float32).astype(jnp.bfloat16)
    key_new = jnp.dot(normed, w_key, preferred_element_type=jnp.float32).astype(jnp.bfloat16)
    value_new = jnp.dot(normed, w_value, preferred_element_type=jnp.float32).astype(jnp.bfloat16)
    log_forget = jax.nn.log_sigmoid(jnp.dot(normed, w_forget, preferred_element_type=jnp.float32) + forget_bias)

    def one_block(index):
        start = index * SEQ_DEV

        def pick(array):
            return lax.dynamic_slice_in_dim(array, start, SEQ_DEV, 0)
        return attend(pick(query), pick(key_new), pick(value_new), pick(log_forget), pick(cache_keys), pick(cache_values), pick(cache_logcum), pick(cache_lengths))
    attended = lax.map(one_block, jnp.arange(N_EP, dtype=jnp.int32)).reshape(seqs, HEADS * HEAD_DIM)
    mixed = stored(tokens.astype(jnp.float32) + jnp.dot(attended, w_attn_out, preferred_element_type=jnp.float32))
    routed_in = normalize(mixed.astype(jnp.float32), expert_norm_gain).astype(jnp.bfloat16)
    flat_ids = expert_ids.reshape(-1)
    rows_all = flat_ids.shape[0]
    room = N_EP * CAP

    def run_expert(outputs, expert):
        chosen = flat_ids == expert
        order = jnp.cumsum(chosen.astype(jnp.int32)) - 1
        where_to = jnp.where(chosen, order, room).astype(jnp.int32)
        source = jnp.zeros((room,), jnp.int32).at[where_to].set(jnp.arange(rows_all, dtype=jnp.int32), mode='drop')
        picked = jnp.take(routed_in, source // TOPK, axis=0)
        answer = expert_unit(picked, w_expert_gate[expert], w_expert_up[expert], w_expert_down[expert])
        filled = jnp.arange(room, dtype=jnp.int32) < jnp.sum(chosen.astype(jnp.int32))
        target = jnp.where(filled, source, rows_all).astype(jnp.int32)
        return (outputs.at[target].set(answer, mode='drop'), None)
    outputs = lax.scan(run_expert, jnp.zeros((rows_all, D), jnp.bfloat16), jnp.arange(EXPERTS, dtype=jnp.int32))[0]
    routed = lax.optimization_barrier(jnp.sum(expert_weights[:, :, None] * outputs.astype(jnp.float32).reshape(seqs, TOPK, D), axis=1))
    gate_dense = jnp.dot(routed_in, w_dense_gate, preferred_element_type=jnp.float32)
    up_dense = jnp.dot(routed_in, w_dense_up, preferred_element_type=jnp.float32)
    units = stored(jax.nn.silu(gate_dense) * up_dense).astype(jnp.float32)
    unit_scale = lax.rsqrt(lax.optimization_barrier(jnp.mean(units * units, axis=1, keepdims=True)) + EPS)
    hidden = (units * unit_scale * dense_norm_gain).astype(jnp.bfloat16)
    dense = jnp.dot(hidden, w_dense_down, preferred_element_type=jnp.float32)
    branch_scale = jax.nn.sigmoid(lax.optimization_barrier(jnp.sum(routed_in.astype(jnp.float32) * branch_gate, axis=1, keepdims=True)))
    return (mixed.astype(jnp.float32) + routed + branch_scale * dense).astype(jnp.bfloat16)
```

```python
import jax
import jax.numpy as jnp
from jax import lax
from jax.sharding import PartitionSpec as P

HEADS = 8
KV_HEADS = 2
HEAD_DIM = 64
TOPK = 6


EPS = 1e-06
LIMIT = 7.0
ALPHA = 1.702


def normalize(values, gain):
    return values * lax.rsqrt(jnp.mean(values * values, axis=-1, keepdims=True) + EPS) * gain


def stored(values):
    return lax.optimization_barrier(values.astype(jnp.bfloat16))


def attend(
    query, key_new, value_new, log_forget, cache_keys, cache_values, cache_logcum, cache_lengths
):
    seqs, length = (cache_keys.shape[0], cache_keys.shape[1])
    group = HEADS // KV_HEADS
    scale = HEAD_DIM ** (-0.5)
    heads_q = query.reshape(seqs, KV_HEADS, group, HEAD_DIM)
    keys = cache_keys.reshape(seqs, length, KV_HEADS, HEAD_DIM)
    values = cache_values.reshape(seqs, length, KV_HEADS, HEAD_DIM)
    own_key = key_new.reshape(seqs, KV_HEADS, HEAD_DIM)
    own_value = value_new.astype(jnp.float32).reshape(seqs, KV_HEADS, 1, HEAD_DIM)
    last_index = jnp.broadcast_to((cache_lengths - 1)[:, None, None], (seqs, HEADS, 1))
    carried = jnp.take_along_axis(cache_logcum, last_index, axis=2)[:, :, 0] + log_forget
    offset = (carried[:, :, None] - cache_logcum).reshape(seqs, KV_HEADS, group, length)
    scores = (
        jnp.einsum("skgd,slkd->skgl", heads_q, keys, preferred_element_type=jnp.float32) * scale
        + offset
    )
    live = jnp.arange(length, dtype=jnp.int32)[None, :] < cache_lengths[:, None]
    scores = jnp.where(live[:, None, None, :], scores, -jnp.inf)
    own = jnp.einsum("skgd,skd->skg", heads_q, own_key, preferred_element_type=jnp.float32) * scale
    top = jnp.maximum(jnp.max(scores, axis=-1), own)
    expo = jnp.exp(scores - top[..., None])
    own_expo = jnp.exp(own - top)
    total = jnp.sum(expo, axis=-1) + own_expo
    weights = (expo / total[..., None]).astype(jnp.bfloat16)
    own_weight = stored(own_expo / total).astype(jnp.float32)
    out = jnp.einsum("skgl,slkd->skgd", weights, values, preferred_element_type=jnp.float32)
    out = out + own_weight[..., None] * own_value
    return out.reshape(seqs, HEADS * HEAD_DIM).astype(jnp.bfloat16)


def split3(values):
    parts = []
    for _ in range(3):
        part = stored(values)
        parts.append(part)
        values = values - part.astype(jnp.float32)
    return parts


def expert_unit(rows, gate_w, up_w, down_w):
    gate = jnp.minimum(jnp.dot(rows, gate_w, preferred_element_type=jnp.float32), LIMIT)
    up = jnp.clip(jnp.dot(rows, up_w, preferred_element_type=jnp.float32), -LIMIT, LIMIT)
    act = ((up + 1.0) * gate * jax.nn.sigmoid(gate * ALPHA)).astype(jnp.bfloat16)
    return jnp.dot(act, down_w, preferred_element_type=jnp.float32).astype(jnp.bfloat16)


def shards(
    tokens,
    attn_norm_gain,
    w_query,
    w_key,
    w_value,
    w_forget,
    forget_bias,
    w_attn_out,
    cache_keys,
    cache_values,
    cache_logcum,
    cache_lengths,
    expert_norm_gain,
    expert_ids,
    expert_weights,
    w_expert_gate,
    w_expert_up,
    w_expert_down,
    w_dense_gate,
    w_dense_up,
    w_dense_down,
    dense_norm_gain,
    branch_gate,
):
    seqs, width = (tokens.shape[0], tokens.shape[1])
    normed = normalize(tokens.astype(jnp.float32), attn_norm_gain).astype(jnp.bfloat16)
    query = jnp.dot(normed, w_query, preferred_element_type=jnp.float32).astype(jnp.bfloat16)
    key_new = jnp.dot(normed, w_key, preferred_element_type=jnp.float32).astype(jnp.bfloat16)
    value_new = jnp.dot(normed, w_value, preferred_element_type=jnp.float32).astype(jnp.bfloat16)
    log_forget = jax.nn.log_sigmoid(
        jnp.dot(normed, w_forget, preferred_element_type=jnp.float32) + forget_bias
    )
    attended = attend(
        query, key_new, value_new, log_forget, cache_keys, cache_values, cache_logcum, cache_lengths
    )
    mixed = stored(
        tokens.astype(jnp.float32)
        + jnp.dot(attended, w_attn_out, preferred_element_type=jnp.float32)
    )
    routed_in = normalize(mixed.astype(jnp.float32), expert_norm_gain).astype(jnp.bfloat16)
    devices = lax.axis_size("ep")
    me = lax.axis_index("ep")
    capacity = max(2, 2 * seqs * TOPK // devices)
    extra = jnp.concatenate(
        [expert_ids.astype(jnp.bfloat16), *split3(expert_weights)], axis=1
    )
    packed = jnp.concatenate([routed_in, jnp.pad(extra, ((0, 0), (0, 128 - 4 * TOPK)))], axis=1)
    everyone = lax.all_gather(packed, "ep", axis=0, tiled=True)
    piece = everyone[:, :width]
    side = everyone[:, width:].astype(jnp.float32)
    ids_all = side[:, :TOPK].astype(jnp.int32)
    weights_all = (
        side[:, TOPK : 2 * TOPK] + side[:, 2 * TOPK : 3 * TOPK] + side[:, 3 * TOPK : 4 * TOPK]
    )
    gate_dense = jnp.dot(piece, w_dense_gate, preferred_element_type=jnp.float32)
    up_dense = jnp.dot(piece, w_dense_up, preferred_element_type=jnp.float32)
    units = stored(jax.nn.silu(gate_dense) * up_dense).astype(jnp.float32)
    squares = lax.psum(jnp.sum(units * units, axis=1), "ep")
    named = ids_all == me
    mine = jnp.sum(jnp.where(named, weights_all, 0.0), axis=1)
    member = jnp.any(named, axis=1).reshape(devices, seqs)
    order = jnp.cumsum(member.astype(jnp.int32), axis=1) - 1
    row = (order + capacity * jnp.arange(devices, dtype=jnp.int32)[:, None]).reshape(-1)
    row = jnp.where(member.reshape(-1), row, -1)
    choose = (row[:, None] == jnp.arange(devices * capacity, dtype=jnp.int32)[None, :]).astype(
        jnp.bfloat16
    )
    arrived = lax.dot_general(
        choose, piece, (((0,), (0,)), ((), ())), preferred_element_type=jnp.float32
    ).astype(jnp.bfloat16)
    answer = expert_unit(arrived, w_expert_gate[0], w_expert_up[0], w_expert_down[0])
    routed = mine[:, None] * jnp.dot(choose, answer, preferred_element_type=jnp.float32)
    units_total = dense_norm_gain.shape[0]
    local = units.shape[1]
    unit_scale = lax.rsqrt(squares / units_total + EPS)
    gain = lax.dynamic_slice_in_dim(dense_norm_gain, me * local, local, 0)
    hidden = (units * unit_scale[:, None] * gain).astype(jnp.bfloat16)
    dense = jnp.dot(hidden, w_dense_down, preferred_element_type=jnp.float32)
    branch_scale = jax.nn.sigmoid(
        jnp.sum(piece.astype(jnp.float32) * branch_gate, axis=1, keepdims=True)
    )
    partial = (routed + branch_scale * dense).astype(jnp.bfloat16)
    total = lax.psum_scatter(partial, "ep", scatter_dimension=0, tiled=True)
    return (mixed.astype(jnp.float32) + total.astype(jnp.float32)).astype(jnp.bfloat16)


def solution(mesh):
    in_specs = (
        P("ep", None),
        P(),
        P(),
        P(),
        P(),
        P(),
        P(),
        P(),
        P("ep", None, None),
        P("ep", None, None),
        P("ep", None, None),
        P("ep"),
        P(),
        P("ep", None),
        P("ep", None),
        P("ep", None, None),
        P("ep", None, None),
        P("ep", None, None),
        P(None, "ep"),
        P(None, "ep"),
        P("ep", None),
        P(),
        P(),
    )
    out_specs = P("ep", None)
    return jax.shard_map(shards, mesh=mesh, in_specs=in_specs, out_specs=out_specs, check_vma=False)
```

```python
import functools

import jax
import jax.numpy as jnp
from jax import lax
from jax.experimental import pallas as pl
from jax.experimental.pallas import tpu as pltpu
from jax.sharding import PartitionSpec as P

HEADS = 8
KV_HEADS = 2
HEAD_DIM = 64
TOPK = 6


EPS = 1e-06
LIMIT = 7.0
ALPHA = 1.702


def normalize(values, gain):
    return values * lax.rsqrt(jnp.mean(values * values, axis=-1, keepdims=True) + EPS) * gain


def stored(values):
    return lax.optimization_barrier(values.astype(jnp.bfloat16))


def front_body(
    lengths,
    tokens,
    gain_ref,
    w_query,
    w_key,
    w_value,
    w_forget,
    bias,
    w_out,
    gain_next,
    keys,
    values,
    logcum,
    mixed_ref,
    routed_ref,
    query_s,
    key_s,
    value_s,
    forget_s,
    attended_s,
):
    step = pl.program_id(0)
    batch, length, pair = keys.shape
    rows = jnp.float32
    group = HEADS // KV_HEADS
    tiles = HEADS * HEAD_DIM // pair

    @pl.when(step == 0)
    def _():
        normed = normalize(tokens[...].astype(rows), gain_ref[...]).astype(jnp.bfloat16)
        for weight, kept in ((w_key, key_s), (w_value, value_s)):
            product = jnp.dot(normed, weight[...], preferred_element_type=rows)
            kept[...] = product.astype(jnp.bfloat16).astype(rows)
        product = jnp.dot(normed, w_query[...], preferred_element_type=rows)
        product = product.astype(jnp.bfloat16).astype(rows)
        for tile in range(tiles):
            query_s[tile] = product[:, tile * pair : (tile + 1) * pair]
        forget = lax.dot_general(
            w_forget[...], normed, (((1,), (1,)), ((), ())), preferred_element_type=rows
        )
        forget = forget + bias[...]
        forget_s[...] = jnp.minimum(forget, 0.0) - jnp.log1p(jnp.exp(-jnp.abs(forget)))

    lane = lax.broadcasted_iota(jnp.int32, (HEADS, pair), 1)
    head = lax.broadcasted_iota(jnp.int32, (HEADS, pair), 0)
    odd = lane // HEAD_DIM
    place = head // group
    seq_lane = lax.broadcasted_iota(jnp.int32, forget_s.shape, 1)
    position = lax.broadcasted_iota(jnp.int32, (HEADS, length), 1)
    scale = HEAD_DIM ** (-0.5)
    for item in range(batch):
        seq = step * batch + item
        stay = jnp.zeros((HEADS, pair), rows)
        move = jnp.zeros((HEADS, pair), rows)
        for tile in range(tiles):
            piece = jnp.broadcast_to(
                query_s[tile, pl.ds(seq, 1), :], (HEADS, pair)
            )
            own_lanes = head == 2 * tile + odd
            stay = jnp.where(own_lanes & (odd == place), piece, stay)
            move = jnp.where(own_lanes & (odd != place), piece, move)
        query = stay + pltpu.roll(move, HEAD_DIM, 1)
        own = jnp.sum(query * key_s[pl.ds(seq, 1), :], axis=1, keepdims=True) * scale
        forget = jnp.sum(jnp.where(seq_lane == seq, forget_s[...], 0.0), axis=1, keepdims=True)
        cum = logcum[item]
        live_count = lengths[seq]
        last = jnp.sum(jnp.where(position == live_count - 1, cum, 0.0), axis=1, keepdims=True)
        scores = lax.dot_general(
            query.astype(jnp.bfloat16),
            keys[item],
            (((1,), (1,)), ((), ())),
            preferred_element_type=rows,
        )
        scores = scores * scale + ((last + forget) - cum)
        scores = jnp.where(position < live_count, scores, -jnp.inf)
        top = jnp.maximum(jnp.max(scores, axis=1, keepdims=True), own)
        expo = jnp.exp(scores - top)
        own_expo = jnp.exp(own - top)
        total = jnp.sum(expo, axis=1, keepdims=True) + own_expo
        weights = (expo / total).astype(jnp.bfloat16)
        own_weight = (own_expo / total).astype(jnp.bfloat16).astype(rows)
        out = jnp.dot(weights, values[item], preferred_element_type=rows)
        out = out + own_weight * value_s[pl.ds(seq, 1), :]
        turned = pltpu.roll(out, HEAD_DIM, 1)
        for tile in range(tiles):
            own_lanes = head == 2 * tile + odd
            part = jnp.where(own_lanes, jnp.where(odd == place, out, turned), 0.0)
            attended_s[tile, pl.ds(seq, 1), :] = jnp.sum(part, axis=0, keepdims=True)

    @pl.when(step == pl.num_programs(0) - 1)
    def _():
        attended = jnp.concatenate([attended_s[tile] for tile in range(tiles)], axis=1)
        attended = attended.astype(jnp.bfloat16)
        mixed = tokens[...].astype(rows) + jnp.dot(
            attended, w_out[...], preferred_element_type=rows
        )
        mixed = mixed.astype(jnp.bfloat16)
        mixed_ref[...] = mixed
        routed_ref[...] = normalize(mixed.astype(rows), gain_next[...]).astype(jnp.bfloat16)


def front(
    tokens, gain, w_query, w_key, w_value, w_forget, bias, w_out, keys, values, logcum, lengths, gain_next
):
    seqs, width = tokens.shape
    batch = max(size for size in (1, 2, 3) if seqs % size == 0)
    pair = keys.shape[2]

    def whole(*shape):
        return pl.BlockSpec(shape, lambda i, *_: (0,) * len(shape))

    def each(*shape):
        return pl.BlockSpec((batch, *shape), lambda i, *_: (i, 0, 0))

    small = (
        tokens,
        gain[None, :],
        w_query,
        w_key,
        w_value,
        w_forget.T,
        bias[:, None],
        w_out,
        gain_next[None, :],
    )
    kept = jax.ShapeDtypeStruct((seqs, width), jnp.bfloat16)
    return pl.pallas_call(
        front_body,
        out_shape=(kept, kept),
        grid_spec=pltpu.PrefetchScalarGridSpec(
            num_scalar_prefetch=1,
            grid=(seqs // batch,),
            in_specs=[whole(*array.shape) for array in small]
            + [each(*keys.shape[1:]), each(*values.shape[1:]), each(*logcum.shape[1:])],
            out_specs=[whole(seqs, width)] * 2,
            scratch_shapes=[
                pltpu.VMEM((HEADS * HEAD_DIM // pair, seqs, pair), jnp.float32),
                pltpu.VMEM((seqs, pair), jnp.float32),
                pltpu.VMEM((seqs, pair), jnp.float32),
                pltpu.VMEM((HEADS, seqs), jnp.float32),
                pltpu.VMEM((HEADS * HEAD_DIM // pair, seqs, pair), jnp.float32),
            ],
        ),
        compiler_params=pltpu.CompilerParams(
            dimension_semantics=("arbitrary",), vmem_limit_bytes=40 * 1024 * 1024
        ),
        cost_estimate=pl.CostEstimate(
            flops=10**9, bytes_accessed=16 * 10**6, transcendentals=2 * 10**5
        ),
        name="front",
    )(lengths, *small, keys, values, logcum)


def split3(values):
    parts = []
    for _ in range(3):
        part = stored(values)
        parts.append(part)
        values = values - part.astype(jnp.float32)
    return parts


def expert_unit(rows, gate_w, up_w, down_w):
    gate = jnp.minimum(jnp.dot(rows, gate_w, preferred_element_type=jnp.float32), LIMIT)
    up = jnp.clip(jnp.dot(rows, up_w, preferred_element_type=jnp.float32), -LIMIT, LIMIT)
    act = ((up + 1.0) * gate * jax.nn.sigmoid(gate * ALPHA)).astype(jnp.bfloat16)
    return jnp.dot(act, down_w, preferred_element_type=jnp.float32).astype(jnp.bfloat16)


def reach(source, target, sent, landed, device):
    return pltpu.make_async_remote_copy(
        src_ref=source,
        dst_ref=target,
        send_sem=sent,
        recv_sem=landed,
        device_id=(device,),
        device_id_type=pl.DeviceIdType.MESH,
    )


def to_row(column, same):
    return jnp.sum(jnp.where(same, column, 0.0), axis=0, keepdims=True)


def to_column(row, same):
    return jnp.sum(jnp.where(same, row, 0.0), axis=1, keepdims=True)


def rest_body(
    units_total,
    packed,
    mixed,
    w_gate,
    w_up,
    w_down,
    d_gate,
    d_up,
    d_down,
    gain,
    branch,
    out,
    rows_s,
    units_s,
    answer_s,
    coef_s,
    square_s,
    squares_s,
    theirs_s,
    joint_s,
    final_s,
    own_sem,
    ag_send,
    ag_recv,
    fw_send,
    fw_recv,
    sq_send,
    sq_recv,
    d2d_send,
    d2d_recv,
    rs_send,
    rs_recv,
):
    kind = jnp.float32
    n = squares_s.shape[0]
    chips = n // 2
    pad = packed.shape[0]
    width = out.shape[1]
    chunk = units_s.shape[1] // pad
    halves = chips // chunk
    size = chunk * pad
    me = lax.axis_index("ep")
    core = lax.rem(me, 2)
    chip = me // 2
    other = chip * 2 + 1 - core
    mine = core * chips
    peer = (1 - core) * chips

    barrier = pltpu.get_barrier_semaphore()

    @pl.loop(1, n)
    def _(k):
        pl.semaphore_signal(
            barrier,
            inc=1,
            device_id=(lax.rem(me + k, n),),
            device_id_type=pl.DeviceIdType.MESH,
        )

    pl.semaphore_wait(barrier, n - 1)

    def ahead(k):
        return lax.rem(chip + k, chips)

    def behind(k):
        return lax.rem(chip - k + chips, chips)

    def gather(k):
        return reach(
            packed, rows_s.at[mine + chip], ag_send.at[k], ag_recv.at[k], ahead(k) * 2 + core
        )

    def landed(k):
        slot = rows_s.at[mine + behind(k)]
        return reach(packed, slot, ag_send.at[k], ag_recv.at[k], behind(k) * 2 + core)

    def forward(k):
        slot = rows_s.at[mine + behind(k)]
        return reach(slot, slot, fw_send.at[k], fw_recv.at[k], other)

    def forwarded(k):
        slot = rows_s.at[peer + behind(k)]
        return reach(slot, slot, fw_send.at[k], fw_recv.at[k], other)

    keep = pltpu.make_async_copy(packed, rows_s.at[mine + chip], own_sem)
    keep.start()

    @pl.loop(1, chips)
    def _(k):
        gather(k).start()

    keep.wait()
    forward(0).start()

    @pl.loop(1, chips)
    def _(k):
        landed(k).wait_recv()
        forward(k).start()

    @pl.loop(0, chips)
    def _(k):
        forwarded(k).wait_recv()

    first = lax.broadcasted_iota(jnp.int32, (size, size), 0)
    second = lax.broadcasted_iota(jnp.int32, (size, size), 1)
    same = first == second

    def load(at):
        block = rows_s[pl.ds(at * chunk, chunk)]
        return block.astype(kind).reshape(size, block.shape[2])

    @pl.loop(0, 2 * halves)
    def _(at):
        wide = load(at)
        block = wide[:, :width].astype(jnp.bfloat16)
        gate = jnp.dot(block, d_gate[...], preferred_element_type=kind)
        up = jnp.dot(block, d_up[...], preferred_element_type=kind)
        units = (gate * jax.nn.sigmoid(gate) * up).astype(jnp.bfloat16).astype(kind)
        units_s[at] = units
        square_s[at] = to_row(jnp.sum(units * units, axis=1, keepdims=True), same)
        side = wide[:, width:]
        lane = lax.broadcasted_iota(jnp.int32, side.shape, 1)
        picked = jnp.where((side == me.astype(kind)) & (lane < TOPK), 1.0, 0.0)
        weight = jnp.zeros((size, 1), kind)
        for part in (3, 2, 1):
            moved = pltpu.roll(side, side.shape[1] - part * TOPK, 1)
            weight = weight + jnp.sum(picked * moved, axis=1, keepdims=True)
        branch_scale = jax.nn.sigmoid(
            jnp.sum(wide[:, :width] * branch[...], axis=1, keepdims=True)
        )
        coef_s[at] = jnp.where(lane == 0, weight, branch_scale)

    def share(k):
        return reach(
            square_s, squares_s.at[k], sq_send.at[k], sq_recv.at[k], lax.rem(me + k, n)
        )

    @pl.loop(1, n)
    def _(k):
        share(k).start()

    @pl.loop(0, 2 * halves)
    def _(at):
        block = load(at)[:, :width].astype(jnp.bfloat16)
        answer_s[at] = expert_unit(block, w_gate[...], w_up[...], w_down[...])

    @pl.loop(1, n)
    def _(k):
        share(k).wait_recv()

    squares_s[0] = square_s[...]
    totals = jnp.sum(squares_s[...], axis=0)
    square_rows = lax.rsqrt(totals / units_total + EPS)
    squares_s[0] = square_rows

    def partial(at):
        scale = to_column(squares_s[0, at], same)
        hidden = (units_s[at] * scale * gain[...]).astype(jnp.bfloat16)
        dense = jnp.dot(hidden, d_down[...], preferred_element_type=kind)
        coef = coef_s[at]
        routed = coef[:, 0:1] * answer_s[at].astype(kind)
        return (routed + coef[:, 1:2] * dense).reshape(chunk, pad, width)

    def cross(half):
        part = pl.ds(half * chunk, chunk)
        return reach(theirs_s.at[part], joint_s.at[part], d2d_send.at[half], d2d_recv.at[half], other)

    def back(k):
        to = behind(k)
        return reach(joint_s.at[to], final_s.at[k], rs_send.at[k], rs_recv.at[k], to * 2 + core)

    @pl.loop(0, halves)
    def _(half):
        theirs_s[pl.ds(half * chunk, chunk)] = partial((1 - core) * halves + half).astype(
            jnp.bfloat16
        )
        cross(half).start()

    @pl.loop(0, halves)
    def _(half):
        part = pl.ds(half * chunk, chunk)
        own = partial(core * halves + half)
        cross(half).wait_recv()
        joint_s[part] = (own + joint_s[part].astype(kind)).astype(jnp.bfloat16)

    @pl.loop(1, chips)
    def _(k):
        back(k).start()

    @pl.loop(1, chips)
    def _(k):
        back(k).wait_recv()

    total = joint_s[chip].astype(kind)
    for k in range(1, chips):
        total = total + final_s[k].astype(kind)
    result = mixed[...].astype(kind) + total[: mixed.shape[0]]
    out[...] = result.astype(jnp.bfloat16)

    @pl.loop(1, chips)
    def _(k):
        gather(k).wait_send()
        back(k).wait_send()

    @pl.loop(0, chips)
    def _(k):
        forward(k).wait_send()

    @pl.loop(1, n)
    def _(k):
        share(k).wait_send()

    @pl.loop(0, halves)
    def _(half):
        cross(half).wait_send()


def rest(n, packed, mixed, w_gate, w_up, w_down, d_gate, d_up, d_down, gain, branch, units_total):
    pad = packed.shape[0]
    width = mixed.shape[1]
    local = d_gate.shape[1]
    chips = n // 2
    chunk = max(size for size in (1, 2, 4, 8) if chips % size == 0)
    halves = chips // chunk
    size = chunk * pad
    half_type = jnp.bfloat16
    vmem = pl.BlockSpec(memory_space=pltpu.VMEM)
    dma = pltpu.SemaphoreType.DMA
    return pl.pallas_call(
        functools.partial(rest_body, units_total),
        out_shape=jax.ShapeDtypeStruct(mixed.shape, half_type),
        in_specs=[vmem] * 10,
        out_specs=vmem,
        scratch_shapes=[
            pltpu.VMEM((n, *packed.shape), half_type),
            pltpu.VMEM((2 * halves, size, local), jnp.float32),
            pltpu.VMEM((2 * halves, size, width), half_type),
            pltpu.VMEM((2 * halves, size, 128), jnp.float32),
            pltpu.VMEM((2 * halves, 1, size), jnp.float32),
            pltpu.VMEM((n, 2 * halves, 1, size), jnp.float32),
            pltpu.VMEM((chips, pad, width), half_type),
            pltpu.VMEM((chips, pad, width), half_type),
            pltpu.VMEM((chips, pad, width), half_type),
            dma,
            dma((chips,)),
            dma((chips,)),
            dma((chips,)),
            dma((chips,)),
            dma((n,)),
            dma((n,)),
            dma((halves,)),
            dma((halves,)),
            dma((chips,)),
            dma((chips,)),
        ],
        compiler_params=pltpu.CompilerParams(
            collective_id=0, has_side_effects=True, vmem_limit_bytes=62 * 1024 * 1024
        ),
        name="rest",
    )(packed, mixed, w_gate, w_up, w_down, d_gate, d_up, d_down, gain, branch)


def shards(
    tokens,
    attn_norm_gain,
    w_query,
    w_key,
    w_value,
    w_forget,
    forget_bias,
    w_attn_out,
    cache_keys,
    cache_values,
    cache_logcum,
    cache_lengths,
    expert_norm_gain,
    expert_ids,
    expert_weights,
    w_expert_gate,
    w_expert_up,
    w_expert_down,
    w_dense_gate,
    w_dense_up,
    w_dense_down,
    dense_norm_gain,
    branch_gate,
):
    mixed, routed_in = front(
        tokens,
        attn_norm_gain,
        w_query,
        w_key,
        w_value,
        w_forget,
        forget_bias,
        w_attn_out,
        cache_keys,
        cache_values,
        cache_logcum,
        cache_lengths,
        expert_norm_gain,
    )
    n = lax.axis_size("ep")
    me = lax.axis_index("ep")
    seqs = tokens.shape[0]
    extra = jnp.concatenate([expert_ids.astype(jnp.bfloat16), *split3(expert_weights)], axis=1)
    packed = jnp.concatenate([routed_in, jnp.pad(extra, ((0, 0), (0, 128 - 4 * TOPK)))], axis=1)
    packed = jnp.pad(packed, ((0, -seqs % 8), (0, 0)))
    local = w_dense_gate.shape[1]
    gain = lax.dynamic_slice_in_dim(dense_norm_gain, me * local, local, 0)
    return rest(
        n,
        packed,
        mixed,
        w_expert_gate[0],
        w_expert_up[0],
        w_expert_down[0],
        w_dense_gate,
        w_dense_up,
        w_dense_down,
        gain[None, :],
        branch_gate[None, :],
        dense_norm_gain.shape[0],
    )


def solution(mesh):
    in_specs = (
        P("ep", None),
        P(),
        P(),
        P(),
        P(),
        P(),
        P(),
        P(),
        P("ep", None, None),
        P("ep", None, None),
        P("ep", None, None),
        P("ep"),
        P(),
        P("ep", None),
        P("ep", None),
        P("ep", None, None),
        P("ep", None, None),
        P("ep", None, None),
        P(None, "ep"),
        P(None, "ep"),
        P("ep", None),
        P(),
        P(),
    )
    out_specs = P("ep", None)
    return jax.shard_map(shards, mesh=mesh, in_specs=in_specs, out_specs=out_specs, check_vma=False)
```

```python
import functools

import jax
import jax.numpy as jnp
from jax import lax
from jax.experimental import pallas as pl
from jax.experimental.pallas import tpu as pltpu
from jax.sharding import PartitionSpec as P

HEADS = 8
KV_HEADS = 2
HEAD_DIM = 64
TOPK = 6


EPS = 1e-06
LIMIT = 7.0
ALPHA = 1.702


def normalize(values, gain):
    return values * lax.rsqrt(jnp.mean(values * values, axis=-1, keepdims=True) + EPS) * gain


def stored(values):
    return lax.optimization_barrier(values.astype(jnp.bfloat16))


def front_body(
    lengths,
    tokens,
    gain_ref,
    w_query,
    w_key,
    w_value,
    w_forget,
    bias,
    w_out,
    gain_next,
    keys,
    values,
    logcum,
    mixed_ref,
    routed_ref,
    query_s,
    key_s,
    value_s,
    forget_s,
    attended_s,
):
    step = pl.program_id(0)
    batch, length, pair = keys.shape
    rows = jnp.float32
    group = HEADS // KV_HEADS
    tiles = HEADS * HEAD_DIM // pair

    @pl.when(step == 0)
    def _():
        normed = normalize(tokens[...].astype(rows), gain_ref[...]).astype(jnp.bfloat16)
        for weight, kept in ((w_key, key_s), (w_value, value_s)):
            product = jnp.dot(normed, weight[...], preferred_element_type=rows)
            kept[...] = product.astype(jnp.bfloat16).astype(rows)
        product = jnp.dot(normed, w_query[...], preferred_element_type=rows)
        product = product.astype(jnp.bfloat16).astype(rows)
        for tile in range(tiles):
            query_s[tile] = product[:, tile * pair : (tile + 1) * pair]
        forget = lax.dot_general(
            w_forget[...], normed, (((1,), (1,)), ((), ())), preferred_element_type=rows
        )
        forget = forget + bias[...]
        forget_s[...] = jnp.minimum(forget, 0.0) - jnp.log1p(jnp.exp(-jnp.abs(forget)))

    lane = lax.broadcasted_iota(jnp.int32, (HEADS, pair), 1)
    head = lax.broadcasted_iota(jnp.int32, (HEADS, pair), 0)
    odd = lane // HEAD_DIM
    place = head // group
    seq_lane = lax.broadcasted_iota(jnp.int32, forget_s.shape, 1)
    position = lax.broadcasted_iota(jnp.int32, (HEADS, length), 1)
    scale = HEAD_DIM ** (-0.5)
    for item in range(batch):
        seq = step * batch + item
        stay = jnp.zeros((HEADS, pair), rows)
        move = jnp.zeros((HEADS, pair), rows)
        for tile in range(tiles):
            piece = jnp.broadcast_to(
                query_s[tile, pl.ds(seq, 1), :], (HEADS, pair)
            )
            own_lanes = head == 2 * tile + odd
            stay = jnp.where(own_lanes & (odd == place), piece, stay)
            move = jnp.where(own_lanes & (odd != place), piece, move)
        query = stay + pltpu.roll(move, HEAD_DIM, 1)
        own = jnp.sum(query * key_s[pl.ds(seq, 1), :], axis=1, keepdims=True) * scale
        forget = jnp.sum(jnp.where(seq_lane == seq, forget_s[...], 0.0), axis=1, keepdims=True)
        cum = logcum[item]
        live_count = lengths[seq]
        last = jnp.sum(jnp.where(position == live_count - 1, cum, 0.0), axis=1, keepdims=True)
        scores = lax.dot_general(
            query.astype(jnp.bfloat16),
            keys[item],
            (((1,), (1,)), ((), ())),
            preferred_element_type=rows,
        )
        scores = scores * scale + ((last + forget) - cum)
        scores = jnp.where(position < live_count, scores, -jnp.inf)
        top = jnp.maximum(jnp.max(scores, axis=1, keepdims=True), own)
        expo = jnp.exp(scores - top)
        own_expo = jnp.exp(own - top)
        total = jnp.sum(expo, axis=1, keepdims=True) + own_expo
        weights = (expo / total).astype(jnp.bfloat16)
        own_weight = (own_expo / total).astype(jnp.bfloat16).astype(rows)
        out = jnp.dot(weights, values[item], preferred_element_type=rows)
        out = out + own_weight * value_s[pl.ds(seq, 1), :]
        turned = pltpu.roll(out, HEAD_DIM, 1)
        for tile in range(tiles):
            own_lanes = head == 2 * tile + odd
            part = jnp.where(own_lanes, jnp.where(odd == place, out, turned), 0.0)
            attended_s[tile, pl.ds(seq, 1), :] = jnp.sum(part, axis=0, keepdims=True)

    @pl.when(step == pl.num_programs(0) - 1)
    def _():
        attended = jnp.concatenate([attended_s[tile] for tile in range(tiles)], axis=1)
        attended = attended.astype(jnp.bfloat16)
        mixed = tokens[...].astype(rows) + jnp.dot(
            attended, w_out[...], preferred_element_type=rows
        )
        mixed = mixed.astype(jnp.bfloat16)
        mixed_ref[...] = mixed
        routed_ref[...] = normalize(mixed.astype(rows), gain_next[...]).astype(jnp.bfloat16)


def front(
    tokens, gain, w_query, w_key, w_value, w_forget, bias, w_out, keys, values, logcum, lengths, gain_next
):
    seqs, width = tokens.shape
    batch = max(size for size in (1, 2, 3) if seqs % size == 0)
    pair = keys.shape[2]

    def whole(*shape):
        return pl.BlockSpec(shape, lambda i, *_: (0,) * len(shape))

    def each(*shape):
        return pl.BlockSpec((batch, *shape), lambda i, *_: (i, 0, 0))

    small = (
        tokens,
        gain[None, :],
        w_query,
        w_key,
        w_value,
        w_forget.T,
        bias[:, None],
        w_out,
        gain_next[None, :],
    )
    kept = jax.ShapeDtypeStruct((seqs, width), jnp.bfloat16)
    return pl.pallas_call(
        front_body,
        out_shape=(kept, kept),
        grid_spec=pltpu.PrefetchScalarGridSpec(
            num_scalar_prefetch=1,
            grid=(seqs // batch,),
            in_specs=[whole(*array.shape) for array in small]
            + [each(*keys.shape[1:]), each(*values.shape[1:]), each(*logcum.shape[1:])],
            out_specs=[whole(seqs, width)] * 2,
            scratch_shapes=[
                pltpu.VMEM((HEADS * HEAD_DIM // pair, seqs, pair), jnp.float32),
                pltpu.VMEM((seqs, pair), jnp.float32),
                pltpu.VMEM((seqs, pair), jnp.float32),
                pltpu.VMEM((HEADS, seqs), jnp.float32),
                pltpu.VMEM((HEADS * HEAD_DIM // pair, seqs, pair), jnp.float32),
            ],
        ),
        compiler_params=pltpu.CompilerParams(
            dimension_semantics=("arbitrary",), vmem_limit_bytes=40 * 1024 * 1024
        ),
        cost_estimate=pl.CostEstimate(
            flops=10**9, bytes_accessed=16 * 10**6, transcendentals=2 * 10**5
        ),
        name="front",
    )(lengths, *small, keys, values, logcum)


def split3(values):
    parts = []
    for _ in range(3):
        part = stored(values)
        parts.append(part)
        values = values - part.astype(jnp.float32)
    return parts


def expert_unit(rows, gate_w, up_w, down_w):
    gate = jnp.minimum(jnp.dot(rows, gate_w, preferred_element_type=jnp.float32), LIMIT)
    up = jnp.clip(jnp.dot(rows, up_w, preferred_element_type=jnp.float32), -LIMIT, LIMIT)
    act = ((up + 1.0) * gate * jax.nn.sigmoid(gate * ALPHA)).astype(jnp.bfloat16)
    return jnp.dot(act, down_w, preferred_element_type=jnp.float32).astype(jnp.bfloat16)


def reach(source, target, sent, landed, device):
    return pltpu.make_async_remote_copy(
        src_ref=source,
        dst_ref=target,
        send_sem=sent,
        recv_sem=landed,
        device_id=(device,),
        device_id_type=pl.DeviceIdType.MESH,
    )


def to_row(column, same):
    return jnp.sum(jnp.where(same, column, 0.0), axis=0, keepdims=True)


def to_column(row, same):
    return jnp.sum(jnp.where(same, row, 0.0), axis=1, keepdims=True)


def rest_body(
    units_total,
    plane,
    packed,
    mixed,
    w_gate,
    w_up,
    w_down,
    d_gate,
    d_up,
    d_down,
    gain,
    branch,
    out,
    rows_s,
    units_s,
    answer_s,
    coef_s,
    square_s,
    squares_s,
    theirs_s,
    joint_s,
    final_s,
    own_sem,
    ag_send,
    ag_recv,
    fw_send,
    fw_recv,
    sq_send,
    sq_recv,
    d2d_send,
    d2d_recv,
    rs_send,
    rs_recv,
):
    kind = jnp.float32
    n = squares_s.shape[0]
    chips = n // 2
    pad = packed.shape[0]
    width = out.shape[1]
    chunk = units_s.shape[1] // pad
    halves = chips // chunk
    size = chunk * pad
    me = lax.axis_index("ep")
    core = lax.rem(me, 2)
    chip = me // 2
    other = chip * 2 + 1 - core
    mine = core * chips
    peer = (1 - core) * chips

    barrier = pltpu.get_barrier_semaphore()

    @pl.loop(1, n)
    def _(k):
        pl.semaphore_signal(
            barrier,
            inc=1,
            device_id=(lax.rem(me + k, n),),
            device_id_type=pl.DeviceIdType.MESH,
        )

    pl.semaphore_wait(barrier, n - 1)

    deep = chips // plane
    level = chip // plane
    spot = lax.rem(chip, plane)

    def before(dz, dp):
        return lax.rem(level - dz + deep, deep) * plane + lax.rem(spot - dp + plane, plane)

    def along(dz):
        to = lax.rem(level + dz, deep) * plane + spot
        k = dz * plane
        return reach(packed, rows_s.at[mine + chip], ag_send.at[k], ag_recv.at[k], to * 2 + core)

    def across(dz, dp):
        to = level * plane + lax.rem(spot + dp, plane)
        k = dz * plane + dp
        slot = rows_s.at[mine + before(dz, 0)]
        return reach(slot, slot, ag_send.at[k], ag_recv.at[k], to * 2 + core)

    def landed(dz, dp):
        slot = rows_s.at[mine + before(dz, dp)]
        k = dz * plane + dp
        return reach(slot, slot, ag_send.at[k], ag_recv.at[k], before(0, dp) * 2 + core)

    def forward(dz, dp):
        slot = rows_s.at[mine + before(dz, dp)]
        k = dz * plane + dp
        return reach(slot, slot, fw_send.at[k], fw_recv.at[k], other)

    def forwarded(dz, dp):
        slot = rows_s.at[peer + before(dz, dp)]
        k = dz * plane + dp
        return reach(slot, slot, fw_send.at[k], fw_recv.at[k], other)

    keep = pltpu.make_async_copy(packed, rows_s.at[mine + chip], own_sem)
    keep.start()

    @pl.loop(1, deep)
    def _(dz):
        along(dz).start()

    keep.wait()

    @pl.loop(1, plane)
    def _(dp):
        across(0, dp).start()

    forward(0, 0).start()

    @pl.loop(1, deep)
    def _(dz):
        landed(dz, 0).wait_recv()

        @pl.loop(1, plane)
        def _(dp):
            across(dz, dp).start()

        forward(dz, 0).start()

    @pl.loop(0, deep)
    def _(dz):
        @pl.loop(1, plane)
        def _(dp):
            landed(dz, dp).wait_recv()
            forward(dz, dp).start()

    @pl.loop(0, deep)
    def _(dz):
        @pl.loop(0, plane)
        def _(dp):
            forwarded(dz, dp).wait_recv()

    first = lax.broadcasted_iota(jnp.int32, (size, size), 0)
    second = lax.broadcasted_iota(jnp.int32, (size, size), 1)
    same = first == second

    def load(at):
        block = rows_s[pl.ds(at * chunk, chunk)]
        return block.astype(kind).reshape(size, block.shape[2])

    @pl.loop(0, 2 * halves)
    def _(at):
        wide = load(at)
        block = wide[:, :width].astype(jnp.bfloat16)
        gate = jnp.dot(block, d_gate[...], preferred_element_type=kind)
        up = jnp.dot(block, d_up[...], preferred_element_type=kind)
        units = (gate * jax.nn.sigmoid(gate) * up).astype(jnp.bfloat16).astype(kind)
        units_s[at] = units
        square_s[at] = to_row(jnp.sum(units * units, axis=1, keepdims=True), same)
        side = wide[:, width:]
        lane = lax.broadcasted_iota(jnp.int32, side.shape, 1)
        picked = jnp.where((side == me.astype(kind)) & (lane < TOPK), 1.0, 0.0)
        weight = jnp.zeros((size, 1), kind)
        for part in (3, 2, 1):
            moved = pltpu.roll(side, side.shape[1] - part * TOPK, 1)
            weight = weight + jnp.sum(picked * moved, axis=1, keepdims=True)
        branch_scale = jax.nn.sigmoid(
            jnp.sum(wide[:, :width] * branch[...], axis=1, keepdims=True)
        )
        coef_s[at] = jnp.where(lane == 0, weight, branch_scale)

    def share(k):
        return reach(
            square_s, squares_s.at[k], sq_send.at[k], sq_recv.at[k], lax.rem(me + k, n)
        )

    @pl.loop(1, n)
    def _(k):
        share(k).start()

    @pl.loop(0, 2 * halves)
    def _(at):
        block = load(at)[:, :width].astype(jnp.bfloat16)
        answer_s[at] = expert_unit(block, w_gate[...], w_up[...], w_down[...])

    @pl.loop(1, n)
    def _(k):
        share(k).wait_recv()

    squares_s[0] = square_s[...]
    totals = jnp.sum(squares_s[...], axis=0)
    square_rows = lax.rsqrt(totals / units_total + EPS)
    squares_s[0] = square_rows

    def partial(at):
        scale = to_column(squares_s[0, at], same)
        hidden = (units_s[at] * scale * gain[...]).astype(jnp.bfloat16)
        dense = jnp.dot(hidden, d_down[...], preferred_element_type=kind)
        coef = coef_s[at]
        routed = coef[:, 0:1] * answer_s[at].astype(kind)
        return (routed + coef[:, 1:2] * dense).reshape(chunk, pad, width)

    def cross(half):
        part = pl.ds(half * chunk, chunk)
        return reach(theirs_s.at[part], joint_s.at[part], d2d_send.at[half], d2d_recv.at[half], other)

    def back(dz, dp):
        k = dz * plane + dp
        slot = joint_s.at[before(dz, dp)]
        return reach(slot, final_s.at[k], rs_send.at[k], rs_recv.at[k], before(0, dp) * 2 + core)

    def down(dz):
        k = dz * plane
        to = before(dz, 0)
        return reach(joint_s.at[to], final_s.at[k], rs_send.at[k], rs_recv.at[k], to * 2 + core)

    def collected(dz):
        total = joint_s[before(dz, 0)].astype(kind)
        for dp in range(1, plane):
            back(dz, dp).wait_recv()
            total = total + final_s[dz * plane + dp].astype(kind)
        return total

    @pl.loop(0, halves)
    def _(half):
        theirs_s[pl.ds(half * chunk, chunk)] = partial((1 - core) * halves + half).astype(
            jnp.bfloat16
        )
        cross(half).start()

    @pl.loop(0, halves)
    def _(half):
        part = pl.ds(half * chunk, chunk)
        own = partial(core * halves + half)
        cross(half).wait_recv()
        joint_s[part] = (own + joint_s[part].astype(kind)).astype(jnp.bfloat16)

    @pl.loop(1, deep + 1)
    def _(step):
        @pl.loop(1, plane)
        def _(dp):
            back(lax.rem(step, deep), dp).start()

    @pl.loop(1, deep)
    def _(dz):
        joint_s[before(dz, 0)] = collected(dz).astype(jnp.bfloat16)
        down(dz).start()

    total = collected(0)
    for dz in range(1, deep):
        down(dz).wait_recv()
        total = total + final_s[dz * plane].astype(kind)
    result = mixed[...].astype(kind) + total[: mixed.shape[0]]
    out[...] = result.astype(jnp.bfloat16)

    @pl.loop(1, deep)
    def _(dz):
        along(dz).wait_send()
        down(dz).wait_send()

    @pl.loop(0, deep)
    def _(dz):
        forward(dz, 0).wait_send()

        @pl.loop(1, plane)
        def _(dp):
            across(dz, dp).wait_send()
            back(dz, dp).wait_send()
            forward(dz, dp).wait_send()

    @pl.loop(1, n)
    def _(k):
        share(k).wait_send()

    @pl.loop(0, halves)
    def _(half):
        cross(half).wait_send()


def rest(n, packed, mixed, w_gate, w_up, w_down, d_gate, d_up, d_down, gain, branch, units_total):
    pad = packed.shape[0]
    width = mixed.shape[1]
    local = d_gate.shape[1]
    chips = n // 2
    chunk = max(size for size in (1, 2, 4, 8) if chips % size == 0)
    halves = chips // chunk
    plane = chips // 4 if chips % 4 == 0 else chips
    size = chunk * pad
    half_type = jnp.bfloat16
    vmem = pl.BlockSpec(memory_space=pltpu.VMEM)
    dma = pltpu.SemaphoreType.DMA
    return pl.pallas_call(
        functools.partial(rest_body, units_total, plane),
        out_shape=jax.ShapeDtypeStruct(mixed.shape, half_type),
        in_specs=[vmem] * 10,
        out_specs=vmem,
        scratch_shapes=[
            pltpu.VMEM((n, *packed.shape), half_type),
            pltpu.VMEM((2 * halves, size, local), jnp.float32),
            pltpu.VMEM((2 * halves, size, width), half_type),
            pltpu.VMEM((2 * halves, size, 128), jnp.float32),
            pltpu.VMEM((2 * halves, 1, size), jnp.float32),
            pltpu.VMEM((n, 2 * halves, 1, size), jnp.float32),
            pltpu.VMEM((chips, pad, width), half_type),
            pltpu.VMEM((chips, pad, width), half_type),
            pltpu.VMEM((chips, pad, width), half_type),
            dma,
            dma((chips,)),
            dma((chips,)),
            dma((chips,)),
            dma((chips,)),
            dma((n,)),
            dma((n,)),
            dma((halves,)),
            dma((halves,)),
            dma((chips,)),
            dma((chips,)),
        ],
        compiler_params=pltpu.CompilerParams(
            collective_id=0, has_side_effects=True, vmem_limit_bytes=62 * 1024 * 1024
        ),
        name="rest",
    )(packed, mixed, w_gate, w_up, w_down, d_gate, d_up, d_down, gain, branch)


def shards(
    tokens,
    attn_norm_gain,
    w_query,
    w_key,
    w_value,
    w_forget,
    forget_bias,
    w_attn_out,
    cache_keys,
    cache_values,
    cache_logcum,
    cache_lengths,
    expert_norm_gain,
    expert_ids,
    expert_weights,
    w_expert_gate,
    w_expert_up,
    w_expert_down,
    w_dense_gate,
    w_dense_up,
    w_dense_down,
    dense_norm_gain,
    branch_gate,
):
    mixed, routed_in = front(
        tokens,
        attn_norm_gain,
        w_query,
        w_key,
        w_value,
        w_forget,
        forget_bias,
        w_attn_out,
        cache_keys,
        cache_values,
        cache_logcum,
        cache_lengths,
        expert_norm_gain,
    )
    n = lax.axis_size("ep")
    me = lax.axis_index("ep")
    seqs = tokens.shape[0]
    extra = jnp.concatenate([expert_ids.astype(jnp.bfloat16), *split3(expert_weights)], axis=1)
    packed = jnp.concatenate([routed_in, jnp.pad(extra, ((0, 0), (0, 128 - 4 * TOPK)))], axis=1)
    packed = jnp.pad(packed, ((0, -seqs % 8), (0, 0)))
    local = w_dense_gate.shape[1]
    gain = lax.dynamic_slice_in_dim(dense_norm_gain, me * local, local, 0)
    return rest(
        n,
        packed,
        mixed,
        w_expert_gate[0],
        w_expert_up[0],
        w_expert_down[0],
        w_dense_gate,
        w_dense_up,
        w_dense_down,
        gain[None, :],
        branch_gate[None, :],
        dense_norm_gain.shape[0],
    )


def solution(mesh):
    in_specs = (
        P("ep", None),
        P(),
        P(),
        P(),
        P(),
        P(),
        P(),
        P(),
        P("ep", None, None),
        P("ep", None, None),
        P("ep", None, None),
        P("ep"),
        P(),
        P("ep", None),
        P("ep", None),
        P("ep", None, None),
        P("ep", None, None),
        P("ep", None, None),
        P(None, "ep"),
        P(None, "ep"),
        P("ep", None),
        P(),
        P(),
    )
    out_specs = P("ep", None)
    return jax.shard_map(shards, mesh=mesh, in_specs=in_specs, out_specs=out_specs, check_vma=False)
```
